32 devices in a mesh: ep: 16 (over z, y, core), tp: 2 (over x).
Axes of the slice: x: 2, y: 2, z: 4, core: 2. Of those that a mesh axis runs over, the one named last changes fastest.
Arguments:
- tokens: bfloat16 [128, 1024], P('ep'), may hold values from -6 to 6
- ssm_state: float32 [128, 32, 64, 128], P('ep', 'tp'), may hold values from -6 to 6
- conv_x: bfloat16 [128, 3, 2048], P('ep', None, 'tp'), may hold values from -6 to 6
- conv_b: bfloat16 [128, 3, 1024], P('ep', None, 'tp'), may hold values from -6 to 6
- conv_c: bfloat16 [128, 3, 1024], P('ep', None, 'tp'), may hold values from -6 to 6
- w_x: bfloat16 [1024, 2048], P(None, 'tp'), may hold values from -0.1875 to 0.1875
- w_z: bfloat16 [1024, 2048], P(None, 'tp'), may hold values from -0.1875 to 0.1875
- w_b: bfloat16 [1024, 1024], P(None, 'tp'), may hold values from -0.1875 to 0.1875
- w_c: bfloat16 [1024, 1024], P(None, 'tp'), may hold values from -0.1875 to 0.1875
- w_dt: bfloat16 [1024, 32], replicated, may hold values from -0.1875 to 0.1875
- dt_bias: float32 [32], P('tp'), may hold values from -2 to 1
- a_log: float32 [32], P('tp'), may hold values from -3 to 1
- d_skip: float32 [32], P('tp'), may hold values from 0.1 to 1.9
- taps_x: bfloat16 [4, 2048], P(None, 'tp'), may hold values from -3 to 3
- taps_b: bfloat16 [4, 1024], P(None, 'tp'), may hold values from -3 to 3
- taps_c: bfloat16 [4, 1024], P(None, 'tp'), may hold values from -3 to 3
- norm1_gain: float32 [1024], replicated, may hold values from 0.1 to 1.9
- group_gain: float32 [2048], P('tp'), may hold values from 0.1 to 1.9
- w_out: bfloat16 [2048, 1024], P('tp'), may hold values from -0.125 to 0.125
- norm2_gain: float32 [1024], replicated, may hold values from 0.1 to 1.9
- route_ids: int32 [128, 6], P('ep'), may hold values from 0 to 15, all different within a row; in each aligned block of 8 rows (0 to 7, 8 to 15, ...) at most 6 rows name the same one
- route_weights: float32 [128, 6], P('ep'), may hold values from 0.1 to 1
- exp_gate: bfloat16 [16, 1024, 512], P('ep', None, 'tp'), may hold values from -0.1875 to 0.1875
- exp_up: bfloat16 [16, 1024, 512], P('ep', None, 'tp'), may hold values from -0.1875 to 0.1875
- exp_down: bfloat16 [16, 512, 1024], P('ep', 'tp'), may hold values from -0.25 to 0.25
- dense_gate: bfloat16 [1024, 1024], P('ep', 'tp'), may hold values from -0.1875 to 0.1875
- dense_up: bfloat16 [1024, 1024], P('ep', 'tp'), may hold values from -0.1875 to 0.1875
- dense_down: bfloat16 [1024, 1024], P('tp', 'ep'), may hold values from -0.1875 to 0.1875
- branch_gate: bfloat16 [1024], replicated, may hold values from -0.375 to 0.375
Outputs:
- mixed: bfloat16 [128, 1024], P('ep', 'tp')
- state_next: float32 [128, 32, 64, 128], P('ep', 'tp')
- conv_x_next: bfloat16 [128, 3, 2048], P('ep', None, 'tp')
- conv_b_next: bfloat16 [128, 3, 1024], P('ep', None, 'tp')
- conv_c_next: bfloat16 [128, 3, 1024], P('ep', None, 'tp')
The draws below stay inside these ranges and needn't reach their ends.
Inputs may be any that keep to these rules, and one draw needn't show every extreme that they name: `route_ids`: each row names 6 different experts. Among the rows of one device no expert is named by more than 6 rows, a bound that some block reaches.
All inputs are finite; a program needn't handle non-finite values.
Results may differ from the reference program's by a relative error of at most 0.019.
Values may be sent and summed in bfloat16 or wider, within the bound.
A program may use at most 64 MiB of HBM per device.

```python
import math
import jax
import jax.numpy as jnp
import numpy as np
from jax import lax

D = 1024
HEADS = 32
HEAD_DIM = 64
STATE_DIM = 128
CONV_TAPS = 4
EXPERT_FF = 512
DENSE_FF = 1024
TOP_K = 6
SEQ_DEV = 8
INNER = 2048
STATE_COLS = 1024
TOKENS = 128
EXPERTS = 16
CAP = 6
N_EP = 16
N_TP = 2


def steps_of(own_key, dims, pieces, least, top_value):
    level, own = 1.0, jax.random.fold_in(own_key, 6)
    for position, parts in pieces:
        draws = jnp.exp(jax.random.uniform(jax.random.fold_in(own, position), (parts,), jnp.float32, least / len(pieces), top_value / len(pieces)))
        level = level * jnp.repeat(draws, dims[position] // parts).reshape([-1 if axis == position else 1 for axis in range(len(dims))])
    return level


def shared_out(stream_key, own, number, rows, amount, top, most, slope):
    order = jax.random.permutation(stream_key, amount)
    heavy_load, ordinary = shares(amount, rows * top, most, slope, True), shares(amount, rows * top, most, slope, False)
    places = jnp.arange(amount)

    def named(sizes, turn):
        used = int((sizes > 0).sum())
        fixed = max(1, used // 4)
        passed = fixed + (places - fixed + turn * (used - fixed)) % max(1, amount - fixed)
        return jnp.zeros((amount,), jnp.int32).at[order[jnp.where(places < fixed, places, passed)]].set(jnp.asarray(sizes, jnp.int32))

    sizes = jnp.where(number % 4 == 0, named(heavy_load, number // 4), named(ordinary, number - number // 4 - 1))
    mixed = jax.random.permutation(jax.random.fold_in(own, 3), amount)
    source_of, receiver = mixed[0:amount // 2 * 2:2], mixed[1:amount // 2 * 2:2]
    margin = jnp.minimum(sizes[source_of] - 1, most - sizes[receiver]) // 2
    margin = jnp.where((source_of == order[0]) | (receiver == order[0]) | (sizes[receiver] == 0), 0, jnp.maximum(margin, 0))
    passed = jax.random.randint(jax.random.fold_in(own, 4), (amount // 2,), 0, 1 << 20) % (margin + 1)
    sizes = sizes.at[source_of].add(-passed).at[receiver].add(passed)
    items = jnp.searchsorted(jnp.cumsum(sizes), jnp.arange(rows * top), side="right").astype(jnp.int32)
    table = items.reshape(top, rows).T
    table = table[jax.random.permutation(jax.random.fold_in(own, 1), rows)]
    turn = jax.random.randint(jax.random.fold_in(own, 2), (rows, 1), 0, top)
    return jnp.take_along_axis(table, (jnp.arange(top)[None, :] + turn) % top, axis=1)


def shares(count, total, bound, slope, full):
    loads = [(1 << 20) // math.isqrt(standing ** slope) + 1 for standing in range(1, count + 1)]
    largest = bound if full else min(bound, max(-(-total // count), total * loads[0] // sum(loads)))
    least = 1 if total - largest >= count - 1 else 0
    holding, surplus = [largest] + [least] * (count - 1), total - largest - least * (count - 1)
    while surplus > 0:
        candidates = [i for i in range(1, count) if holding[i] < largest] or [i for i in range(1, count) if holding[i] < bound]
        mass, left = sum([loads[i] for i in candidates]), surplus
        for i in candidates:
            extra = min(bound - holding[i], max(1, left * loads[i] // mass), surplus)
            holding[i] = holding[i] + extra
            surplus = surplus - extra
    return np.array(holding)


def scatter_about(own_key, shape, scale, most, pieces=(), kind=jnp.bfloat16):
    drawn = jax.random.normal(own_key, shape, jnp.float32) * scale
    if len(pieces) > 0:
        drawn = steps_of(own_key, shape, pieces, -0.22, 0.18) * drawn
    return jnp.clip(drawn, min=-most, max=most).astype(kind)


def setup_inputs(seed: int = 0) -> dict:
    keys = jax.random.split(jax.random.key(seed), 30)
    tokens = scatter_about(keys[0], (TOKENS, D), 1.0, 6.0, ((0, 16),))
    ssm_state = scatter_about(keys[1], (TOKENS, HEADS, HEAD_DIM, STATE_DIM), 1.0, 6.0, ((0, 16), (1, 2)), jnp.float32)
    conv_x = scatter_about(keys[2], (TOKENS, CONV_TAPS - 1, INNER), 1.0, 6.0, ((0, 16), (2, 2)))
    conv_b = scatter_about(keys[3], (TOKENS, CONV_TAPS - 1, STATE_COLS), 1.0, 6.0, ((0, 16), (2, 2)))
    conv_c = scatter_about(keys[4], (TOKENS, CONV_TAPS - 1, STATE_COLS), 1.0, 6.0, ((0, 16), (2, 2)))
    w_x = scatter_about(keys[5], (D, INNER), D ** -0.5, 0.1875, ((1, 2),))
    w_z = scatter_about(keys[6], (D, INNER), D ** -0.5, 0.1875, ((1, 2),))
    w_b = scatter_about(keys[7], (D, STATE_COLS), D ** -0.5, 0.1875, ((1, 2),))
    w_c = scatter_about(keys[8], (D, STATE_COLS), D ** -0.5, 0.1875, ((1, 2),))
    w_dt = scatter_about(keys[9], (D, HEADS), D ** -0.5, 0.1875)
    dt_bias = jnp.clip(-2.0 + 3.0 * jax.random.uniform(keys[10], (HEADS,), jnp.float32) ** steps_of(keys[10], (HEADS,), ((0, 2),), -0.2, 0.2), -2.0, 1.0)
    a_log = jnp.clip(-3.0 + 4.0 * jax.random.uniform(keys[11], (HEADS,), jnp.float32) ** steps_of(keys[11], (HEADS,), ((0, 2),), -0.2, 0.2), -3.0, 1.0)
    d_skip = jnp.clip(1.0 + 0.18 * jax.random.normal(keys[12], (HEADS,), jnp.float32), 0.1, 1.9)
    taps_x = scatter_about(keys[13], (CONV_TAPS, INNER), CONV_TAPS ** -0.5, 3.0, ((1, 2),))
    taps_b = scatter_about(keys[14], (CONV_TAPS, STATE_COLS), CONV_TAPS ** -0.5, 3.0, ((1, 2),))
    taps_c = scatter_about(keys[15], (CONV_TAPS, STATE_COLS), CONV_TAPS ** -0.5, 3.0, ((1, 2),))
    norm1_gain = jnp.clip(1.0 + 0.18 * jax.random.normal(keys[16], (D,), jnp.float32), 0.1, 1.9)
    group_gain = jnp.clip(1.0 + 0.18 * jax.random.normal(keys[17], (INNER,), jnp.float32), 0.1, 1.9)
    w_out = scatter_about(keys[18], (INNER, D), INNER ** -0.5, 0.125, ((0, 2),))
    norm2_gain = jnp.clip(1.0 + 0.18 * jax.random.normal(keys[19], (D,), jnp.float32), 0.1, 1.9)
    route_ids_keys = jax.random.split(jax.random.fold_in(keys[20], 1), TOKENS // SEQ_DEV)
    route_ids_turns = jax.random.permutation(jax.random.fold_in(keys[20], 3), TOKENS // SEQ_DEV)
    route_ids = jax.vmap(lambda own, number: shared_out(jax.random.fold_in(keys[20], 2), own, number, SEQ_DEV, EXPERTS, TOP_K, CAP, 2))(route_ids_keys, route_ids_turns).reshape((TOKENS, TOP_K))
    route_weights = jnp.clip(0.1 + 0.9 * jax.random.uniform(keys[21], (TOKENS, TOP_K), jnp.float32) ** steps_of(keys[21], (TOKENS, TOP_K), ((0, 16),), -0.2, 0.2), 0.1, 1.0)
    exp_gate = scatter_about(keys[22], (EXPERTS, D, EXPERT_FF), D ** -0.5, 0.1875, ((0, 16), (2, 2)))
    exp_up = scatter_about(keys[23], (EXPERTS, D, EXPERT_FF), D ** -0.5, 0.1875, ((0, 16), (2, 2)))
    exp_down = scatter_about(keys[24], (EXPERTS, EXPERT_FF, D), EXPERT_FF ** -0.5, 0.25, ((0, 16), (1, 2)))
    dense_gate = scatter_about(keys[25], (D, DENSE_FF), D ** -0.5, 0.1875, ((0, 16), (1, 2)))
    dense_up = scatter_about(keys[26], (D, DENSE_FF), D ** -0.5, 0.1875, ((0, 16), (1, 2)))
    dense_down = scatter_about(keys[27], (DENSE_FF, D), DENSE_FF ** -0.5, 0.1875, ((0, 2), (1, 16)))
    branch_gate = scatter_about(keys[28], (D,), (D // 4) ** -0.5, 0.375)
    return dict(tokens=tokens, ssm_state=ssm_state, conv_x=conv_x, conv_b=conv_b, conv_c=conv_c, w_x=w_x, w_z=w_z, w_b=w_b, w_c=w_c, w_dt=w_dt, dt_bias=dt_bias, a_log=a_log, d_skip=d_skip, taps_x=taps_x, taps_b=taps_b, taps_c=taps_c, norm1_gain=norm1_gain, group_gain=group_gain, w_out=w_out, norm2_gain=norm2_gain, route_ids=route_ids, route_weights=route_weights, exp_gate=exp_gate, exp_up=exp_up, exp_down=exp_down, dense_gate=dense_gate, dense_up=dense_up, dense_down=dense_down, branch_gate=branch_gate)


epsilon = 1e-06

def rms_rows(values, gain):
    return values * lax.rsqrt(lax.optimization_barrier(jnp.mean(values * values, axis=-1, keepdims=True)) + epsilon) * gain

def blocked_sum(left, right, blocks):
    width = left.shape[1] // blocks
    total = jnp.zeros((left.shape[0], right.shape[1]), jnp.float32)
    for index in range(blocks):
        partial_term = jnp.dot(left[:, index * width:(index + 1) * width], right[index * width:(index + 1) * width], preferred_element_type=jnp.float32)
        rounded = lax.optimization_barrier(partial_term.astype(jnp.bfloat16))
        total = total + rounded.astype(jnp.float32)
    return total

def short_conv(previous, fresh, taps):
    window = jnp.concatenate((previous, fresh[:, None]), axis=1)
    summed = lax.optimization_barrier(jnp.sum(window.astype(jnp.float32) * taps.astype(jnp.float32)[None], axis=1))
    return (jax.nn.silu(summed), window[:, 1:])

def mixer_core(x_new, z_new, b_new, c_new, dt_raw, ssm_state, conv_x, conv_b, conv_c, dt_bias, a_log, d_skip, taps_x, taps_b, taps_c, group_gain):
    seqs, heads, head_dim, state_dim = ssm_state.shape
    groups = b_new.shape[1] // state_dim
    x_conv, conv_x_next = short_conv(conv_x, x_new, taps_x)
    b_conv, conv_b_next = short_conv(conv_b, b_new, taps_b)
    c_conv, conv_c_next = short_conv(conv_c, c_new, taps_c)
    x_heads = x_conv.reshape(seqs, heads, head_dim)
    b_heads = jnp.repeat(b_conv.reshape(seqs, groups, state_dim), heads // groups, axis=1)
    c_heads = jnp.repeat(c_conv.reshape(seqs, groups, state_dim), heads // groups, axis=1)
    step = jax.nn.softplus(dt_raw + dt_bias)
    decay = jnp.exp(-step * jnp.exp(a_log))
    state_next = decay[:, :, None, None] * ssm_state + (step[:, :, None] * x_heads)[:, :, :, None] * b_heads[:, :, None, :]
    readout = jnp.einsum('shpn,shn->shp', state_next, c_heads, precision=lax.Precision.HIGHEST) + d_skip[None, :, None] * x_heads
    gated = readout.reshape(seqs, heads * head_dim) * jax.nn.silu(z_new.astype(jnp.float32))
    grouped = gated.reshape(seqs, groups, -1)
    grouped = grouped * lax.rsqrt(lax.optimization_barrier(jnp.mean(grouped * grouped, axis=-1, keepdims=True)) + epsilon)
    mixed_heads = (grouped.reshape(seqs, heads * head_dim) * group_gain).astype(jnp.bfloat16)
    return (mixed_heads, state_next, conv_x_next, conv_b_next, conv_c_next)

def reference(tokens, ssm_state, conv_x, conv_b, conv_c, w_x, w_z, w_b, w_c, w_dt, dt_bias, a_log, d_skip, taps_x, taps_b, taps_c, norm1_gain, group_gain, w_out, norm2_gain, route_ids, route_weights, exp_gate, exp_up, exp_down, dense_gate, dense_up, dense_down, branch_gate):
    stream = tokens.astype(jnp.float32)
    normed = rms_rows(stream, norm1_gain).astype(jnp.bfloat16)
    x_new = jnp.dot(normed, w_x, preferred_element_type=jnp.float32).astype(jnp.bfloat16)
    z_new = jnp.dot(normed, w_z, preferred_element_type=jnp.float32).astype(jnp.bfloat16)
    b_new = jnp.dot(normed, w_b, preferred_element_type=jnp.float32).astype(jnp.bfloat16)
    c_new = jnp.dot(normed, w_c, preferred_element_type=jnp.float32).astype(jnp.bfloat16)
    dt_raw = jnp.dot(normed, w_dt, preferred_element_type=jnp.float32)
    mixed_heads, state_next, conv_x_next, conv_b_next, conv_c_next = mixer_core(x_new, z_new, b_new, c_new, dt_raw, ssm_state, conv_x, conv_b, conv_c, dt_bias, a_log, d_skip, taps_x, taps_b, taps_c, group_gain)
    residual = (stream + blocked_sum(mixed_heads, w_out, N_TP)).astype(jnp.bfloat16)
    normed2 = rms_rows(residual.astype(jnp.float32), norm2_gain).astype(jnp.bfloat16)
    expert_iota = jnp.arange(EXPERTS, dtype=jnp.int32)
    matches = route_ids[:, :, None] == expert_iota[None, None, :]
    routed = lax.optimization_barrier(jnp.sum(matches.astype(jnp.int32), axis=1))
    weight_of = lax.optimization_barrier(jnp.sum(jnp.where(matches, route_weights[:, :, None], jnp.float32(0.0)), axis=1))
    blocked = routed.reshape(N_EP, SEQ_DEV, EXPERTS)
    ranked = (jnp.cumsum(blocked, axis=1) - blocked).reshape(TOKENS, EXPERTS)
    token_iota = jnp.arange(TOKENS, dtype=jnp.int32)
    source = token_iota // SEQ_DEV
    total_slots = EXPERTS * N_EP * CAP
    target = expert_iota[None, :] * (N_EP * CAP) + source[:, None] * CAP + ranked
    target = jnp.where(routed > 0, target, total_slots).astype(jnp.int32)
    owners = jnp.broadcast_to(token_iota[:, None], (TOKENS, EXPERTS)).reshape(-1)
    slot_token = jnp.zeros((total_slots,), jnp.int32).at[target.reshape(-1)].set(owners, mode='drop')
    slot_weight = jnp.zeros((total_slots,), jnp.float32).at[target.reshape(-1)].set(weight_of.reshape(-1), mode='drop')

    def run_expert(operands):
        index_rows, gate_weight, up_weight, down_weight = operands
        chosen = normed2[index_rows]
        gate_pre = jnp.dot(chosen, gate_weight, preferred_element_type=jnp.float32)
        up_pre = jnp.dot(chosen, up_weight, preferred_element_type=jnp.float32)
        active = (jax.nn.silu(gate_pre) * up_pre).astype(jnp.bfloat16)
        return blocked_sum(active, down_weight, N_TP).astype(jnp.bfloat16)
    slot_out = lax.map(run_expert, (slot_token.reshape(EXPERTS, N_EP * CAP), exp_gate, exp_up, exp_down))
    expert_sum = jnp.zeros((TOKENS, D), jnp.float32).at[slot_token].add(slot_weight[:, None] * slot_out.reshape(total_slots, D).astype(jnp.float32))
    dense_pre = jnp.dot(normed2, dense_gate, preferred_element_type=jnp.float32)
    dense_lift = jnp.dot(normed2, dense_up, preferred_element_type=jnp.float32)
    dense_active = (jax.nn.silu(dense_pre) * dense_lift).astype(jnp.bfloat16)
    dense_out = blocked_sum(dense_active, dense_down, N_TP)
    branch = jax.nn.sigmoid(jnp.dot(normed2, branch_gate[:, None], preferred_element_type=jnp.float32))
    mixed = (residual.astype(jnp.float32) + expert_sum + branch * dense_out).astype(jnp.bfloat16)
    return (mixed, state_next, conv_x_next, conv_b_next, conv_c_next)
```

```python
import functools

import jax
import jax.numpy as jnp
from jax import lax
from jax.experimental import pallas as pl
from jax.experimental.pallas import tpu as pltpu
from jax.sharding import PartitionSpec as P

epsilon = 1e-06


def rms_rows(values, gain):
    return values * lax.rsqrt(jnp.mean(values * values, axis=-1, keepdims=True) + epsilon) * gain


def short_conv(previous, fresh, taps):
    window = jnp.concatenate((previous, fresh[:, None]), axis=1)
    summed = jnp.sum(window.astype(jnp.float32) * taps.astype(jnp.float32)[None], axis=1)
    return (jax.nn.silu(summed), window[:, 1:])


def mixer_core(
    x_new,
    z_new,
    b_new,
    c_new,
    dt_raw,
    ssm_state,
    conv_x,
    conv_b,
    conv_c,
    dt_bias,
    a_log,
    d_skip,
    taps_x,
    taps_b,
    taps_c,
    group_gain,
):
    seqs, heads, head_dim, state_dim = ssm_state.shape
    groups = b_new.shape[1] // state_dim
    x_conv, conv_x_next = short_conv(conv_x, x_new, taps_x)
    b_conv, conv_b_next = short_conv(conv_b, b_new, taps_b)
    c_conv, conv_c_next = short_conv(conv_c, c_new, taps_c)
    x_heads = x_conv.reshape(seqs, heads, head_dim)
    b_heads = jnp.repeat(b_conv.reshape(seqs, groups, state_dim), heads // groups, axis=1)
    c_heads = jnp.repeat(c_conv.reshape(seqs, groups, state_dim), heads // groups, axis=1)
    step = jax.nn.softplus(dt_raw + dt_bias)
    decay = jnp.exp(-step * jnp.exp(a_log))
    state_next = (
        decay[:, :, None, None] * ssm_state
        + (step[:, :, None] * x_heads)[:, :, :, None] * b_heads[:, :, None, :]
    )
    readout = (
        jnp.einsum("shpn,shn->shp", state_next, c_heads, precision=lax.Precision.HIGHEST)
        + d_skip[None, :, None] * x_heads
    )
    gated = readout.reshape(seqs, heads * head_dim) * jax.nn.silu(z_new.astype(jnp.float32))
    grouped = gated.reshape(seqs, groups, -1)
    grouped = grouped * lax.rsqrt(jnp.mean(grouped * grouped, axis=-1, keepdims=True) + epsilon)
    mixed_heads = (grouped.reshape(seqs, heads * head_dim) * group_gain).astype(jnp.bfloat16)
    return (mixed_heads, state_next, conv_x_next, conv_b_next, conv_c_next)


def tail_kernel(
    peers,
    splits,
    share,
    mixed_ref,
    w_out_hbm,
    tokens_ref,
    gain_ref,
    ids_ref,
    weights_ref,
    gate_hbm,
    up_hbm,
    down_hbm,
    stage_ref,
    branch_ref,
    out_ref,
    w_out,
    gate_up,
    down,
    partials,
    features,
    tables,
    dense,
    packed,
    returned,
    load_sem,
    part_send,
    part_recv,
    feat_send,
    feat_recv,
    table_send,
    table_recv,
    dense_send,
    dense_recv,
    ret_send,
    ret_recv,
):
    ep = lax.axis_index("ep")
    tp = lax.axis_index("tp")
    everyone = peers * splits
    me = ep * splits + tp
    seqs, width = tokens_ref.shape
    hidden = down.shape[0]
    part = width // splits

    loads = [
        pltpu.make_async_copy(w_out_hbm, w_out, load_sem.at[0]),
        pltpu.make_async_copy(gate_hbm.at[0], gate_up.at[:, pl.ds(0, hidden)], load_sem.at[1]),
        pltpu.make_async_copy(up_hbm.at[0], gate_up.at[:, pl.ds(hidden, hidden)], load_sem.at[2]),
        pltpu.make_async_copy(down_hbm.at[0], down, load_sem.at[3]),
    ]
    for load in loads:
        load.start()

    barrier = pltpu.get_barrier_semaphore()

    def greet(i, carry):
        other = lax.rem(me + i, everyone)
        pl.semaphore_signal(
            barrier,
            inc=1,
            device_id={"ep": other // splits, "tp": lax.rem(other, splits)},
            device_id_type=pl.DeviceIdType.MESH,
        )
        return carry

    lax.fori_loop(1, everyone, greet, 0)

    lanes = lax.broadcasted_iota(jnp.int32, tables.shape[1:], 1)
    table = jnp.zeros(tables.shape[1:], jnp.float32)
    for k in range(ids_ref.shape[1]):
        table = table + jnp.where(lanes == ids_ref[:, k : k + 1], weights_ref[:, k : k + 1], 0.0)
    tables[ep] = table
    dense[ep] = stage_ref[ep]

    loads[0].wait()
    partial_out = jnp.dot(mixed_ref[...], w_out[...], preferred_element_type=jnp.float32)
    partials[tp] = partial_out.astype(jnp.bfloat16)

    pl.semaphore_wait(barrier, everyone - 1)

    def part_copy(i, slot):
        return pltpu.make_async_remote_copy(
            src_ref=partials.at[slot],
            dst_ref=partials.at[slot],
            send_sem=part_send.at[i],
            recv_sem=part_recv.at[slot],
            device_id={"ep": ep, "tp": lax.rem(tp + i, splits)},
            device_id_type=pl.DeviceIdType.MESH,
        )

    def table_copy(i, slot):
        return pltpu.make_async_remote_copy(
            src_ref=tables.at[slot],
            dst_ref=tables.at[slot],
            send_sem=table_send.at[i],
            recv_sem=table_recv.at[slot],
            device_id={"ep": lax.rem(ep + i, peers), "tp": tp},
            device_id_type=pl.DeviceIdType.MESH,
        )

    def dense_copy(i, slot):
        return pltpu.make_async_remote_copy(
            src_ref=stage_ref.at[lax.rem(ep + i, peers)],
            dst_ref=dense.at[slot],
            send_sem=dense_send.at[i],
            recv_sem=dense_recv.at[slot],
            device_id={"ep": lax.rem(ep + i, peers), "tp": tp},
            device_id_type=pl.DeviceIdType.MESH,
        )

    def feat_copy(i, slot):
        return pltpu.make_async_remote_copy(
            src_ref=features.at[slot],
            dst_ref=features.at[slot],
            send_sem=feat_send.at[i],
            recv_sem=feat_recv.at[slot],
            device_id={"ep": lax.rem(ep + i, peers), "tp": tp},
            device_id_type=pl.DeviceIdType.MESH,
        )

    def ret_copy(i, slot):
        other = lax.rem(me + i, everyone)
        return pltpu.make_async_remote_copy(
            src_ref=packed.at[lax.rem(other, splits), other // splits],
            dst_ref=returned.at[slot],
            send_sem=ret_send.at[i],
            recv_sem=ret_recv.at[slot],
            device_id={"ep": other // splits, "tp": lax.rem(other, splits)},
            device_id_type=pl.DeviceIdType.MESH,
        )

    def start_all(copy, slot, count):
        def step(i, carry):
            copy(i, slot).start()
            return carry

        lax.fori_loop(1, count, step, 0)

    def take_all(copy, own, count):
        def step(i, carry):
            copy(i, lax.rem(own + count - i, count)).wait_recv()
            return carry

        lax.fori_loop(1, count, step, 0)

    def sent_all(copy, slot, count):
        def step(i, carry):
            copy(i, slot).wait_send()
            return carry

        lax.fori_loop(1, count, step, 0)

    start_all(part_copy, tp, splits)
    start_all(table_copy, ep, peers)
    start_all(dense_copy, ep, peers)

    take_all(part_copy, tp, splits)
    summed = partials[0].astype(jnp.float32)
    for t in range(1, splits):
        summed = summed + partials[t].astype(jnp.float32)
    residual = (tokens_ref[...].astype(jnp.float32) + summed).astype(jnp.bfloat16)
    residual = residual.astype(jnp.float32)
    normed2 = rms_rows(residual, gain_ref[...]).astype(jnp.bfloat16)
    features[ep] = normed2
    start_all(feat_copy, ep, peers)

    take_all(table_copy, ep, peers)
    take_all(dense_copy, ep, peers)
    every_table = tables[...].reshape(peers * seqs, tables.shape[2])
    columns = lax.broadcasted_iota(jnp.int32, every_table.shape, 1)
    own_weight = jnp.sum(jnp.where(columns == ep, every_table, 0.0), axis=1, keepdims=True)
    dense_weights = dense[...].reshape(width, dense.shape[2])
    for load in loads[1:]:
        load.wait()

    take_all(feat_copy, ep, peers)
    rows = features[...].astype(jnp.float32).reshape(peers * seqs, width)
    rows16 = rows.astype(jnp.bfloat16)
    pre = jnp.dot(rows16, gate_up[...], preferred_element_type=jnp.float32)
    active = own_weight * (jax.nn.silu(pre[:, :hidden]) * pre[:, hidden:])
    dense_pre = jnp.dot(rows16, dense_weights, preferred_element_type=jnp.float32)
    branch = jax.nn.sigmoid(
        jnp.sum(rows * branch_ref[...].astype(jnp.float32), axis=1, keepdims=True)
    )
    lane = lax.broadcasted_iota(jnp.int32, dense_pre.shape, 1)
    dense_act = jax.nn.silu(pltpu.roll(dense_pre, 2 * share, 1)) * pltpu.roll(dense_pre, share, 1)
    dense_act = jnp.where((lane >= 2 * share) & (lane < 3 * share), branch * dense_act, 0.0)
    total = jnp.dot(active.astype(jnp.bfloat16), down[...], preferred_element_type=jnp.float32)
    total = total + lax.dot_general(
        dense_act.astype(jnp.bfloat16),
        dense_weights,
        (((1,), (1,)), ((), ())),
        preferred_element_type=jnp.float32,
    )
    for t in range(splits):
        packed[t] = (
            total[:, t * part : (t + 1) * part].reshape(peers, seqs, part).astype(jnp.bfloat16)
        )
    returned[me] = packed[tp, ep]
    start_all(ret_copy, me, everyone)

    sent_all(part_copy, tp, splits)
    sent_all(table_copy, ep, peers)
    sent_all(dense_copy, ep, peers)
    sent_all(feat_copy, ep, peers)
    own_rows = residual[:, :part]
    for t in range(1, splits):
        own_rows = jnp.where(tp == t, residual[:, t * part : (t + 1) * part], own_rows)

    take_all(ret_copy, me, everyone)
    mixed = own_rows + jnp.sum(returned[...].astype(jnp.float32), axis=0)
    out_ref[...] = mixed.astype(jnp.bfloat16)
    sent_all(ret_copy, me, everyone)


def after_mixer(
    mixed_heads,
    w_out,
    tokens,
    norm2_gain,
    route_ids,
    route_weights,
    exp_gate,
    exp_up,
    exp_down,
    dense_gate,
    dense_up,
    dense_down,
    branch_gate,
):
    peers = lax.axis_size("ep")
    splits = lax.axis_size("tp")
    seqs, width = tokens.shape
    depth, local_hidden = dense_gate.shape
    share = local_hidden // peers
    hidden = exp_gate.shape[2]
    part = width // splits
    lanes = -(-3 * share // 128) * 128
    by_owner = lambda w: w.reshape(depth, peers, share).transpose(1, 0, 2)
    stage = jnp.concatenate(
        (
            by_owner(dense_gate),
            by_owner(dense_up),
            dense_down.reshape(peers, share, depth).transpose(0, 2, 1),
            jnp.zeros((peers, depth, lanes - 3 * share), jnp.bfloat16),
        ),
        axis=2,
    )
    vmem = pl.BlockSpec(memory_space=pltpu.VMEM)
    hbm = pl.BlockSpec(memory_space=pl.ANY)
    dma = lambda count: pltpu.SemaphoreType.DMA((count,))
    return pl.pallas_call(
        functools.partial(tail_kernel, peers, splits, share),
        out_shape=jax.ShapeDtypeStruct((seqs, part), jnp.bfloat16),
        in_specs=[vmem, hbm, vmem, vmem, vmem, vmem, hbm, hbm, hbm, vmem, vmem],
        out_specs=vmem,
        scratch_shapes=[
            pltpu.VMEM(w_out.shape, jnp.bfloat16),
            pltpu.VMEM((width, 2 * hidden), jnp.bfloat16),
            pltpu.VMEM((hidden, width), jnp.bfloat16),
            pltpu.VMEM((splits, seqs, width), jnp.bfloat16),
            pltpu.VMEM((peers, seqs, width), jnp.bfloat16),
            pltpu.VMEM((peers, seqs, 128), jnp.float32),
            pltpu.VMEM((peers, depth, lanes), jnp.bfloat16),
            pltpu.VMEM((splits, peers, seqs, part), jnp.bfloat16),
            pltpu.VMEM((peers * splits, seqs, part), jnp.bfloat16),
            dma(4),
            dma(splits),
            dma(splits),
            dma(peers),
            dma(peers),
            dma(peers),
            dma(peers),
            dma(peers),
            dma(peers),
            dma(peers * splits),
            dma(peers * splits),
        ],
        compiler_params=pltpu.CompilerParams(
            collective_id=0, has_side_effects=True, vmem_limit_bytes=32 * 1024 * 1024
        ),
        cost_estimate=pl.CostEstimate(flops=10**9, bytes_accessed=10**7, transcendentals=0),
    )(
        mixed_heads,
        w_out,
        tokens,
        norm2_gain[None],
        route_ids,
        route_weights,
        exp_gate,
        exp_up,
        exp_down,
        stage,
        branch_gate[None],
    )


def body(
    tokens,
    ssm_state,
    conv_x,
    conv_b,
    conv_c,
    w_x,
    w_z,
    w_b,
    w_c,
    w_dt,
    dt_bias,
    a_log,
    d_skip,
    taps_x,
    taps_b,
    taps_c,
    norm1_gain,
    group_gain,
    w_out,
    norm2_gain,
    route_ids,
    route_weights,
    exp_gate,
    exp_up,
    exp_down,
    dense_gate,
    dense_up,
    dense_down,
    branch_gate,
):
    stream = tokens.astype(jnp.float32)
    normed = rms_rows(stream, norm1_gain).astype(jnp.bfloat16)
    x_proj = jnp.dot(normed, w_x, preferred_element_type=jnp.float32).astype(jnp.bfloat16)
    z_proj = jnp.dot(normed, w_z, preferred_element_type=jnp.float32).astype(jnp.bfloat16)
    b_proj = jnp.dot(normed, w_b, preferred_element_type=jnp.float32).astype(jnp.bfloat16)
    c_proj = jnp.dot(normed, w_c, preferred_element_type=jnp.float32).astype(jnp.bfloat16)
    local_heads = ssm_state.shape[1]
    dt_columns = lax.dynamic_slice_in_dim(w_dt, lax.axis_index("tp") * local_heads, local_heads, 1)
    dt_raw = jnp.dot(normed, dt_columns, preferred_element_type=jnp.float32)
    mixed_heads, state_next, conv_x_next, conv_b_next, conv_c_next = mixer_core(
        x_proj,
        z_proj,
        b_proj,
        c_proj,
        dt_raw,
        ssm_state,
        conv_x,
        conv_b,
        conv_c,
        dt_bias,
        a_log,
        d_skip,
        taps_x,
        taps_b,
        taps_c,
        group_gain,
    )
    mixed = after_mixer(
        mixed_heads,
        w_out,
        tokens,
        norm2_gain,
        route_ids,
        route_weights,
        exp_gate,
        exp_up,
        exp_down,
        dense_gate,
        dense_up,
        dense_down,
        branch_gate,
    )
    return (mixed, state_next, conv_x_next, conv_b_next, conv_c_next)


def solution(mesh):
    return jax.shard_map(
        body,
        mesh=mesh,
        in_specs=(
            P("ep", None),
            P("ep", "tp", None, None),
            P("ep", None, "tp"),
            P("ep", None, "tp"),
            P("ep", None, "tp"),
            P(None, "tp"),
            P(None, "tp"),
            P(None, "tp"),
            P(None, "tp"),
            P(),
            P("tp"),
            P("tp"),
            P("tp"),
            P(None, "tp"),
            P(None, "tp"),
            P(None, "tp"),
            P(),
            P("tp"),
            P("tp", None),
            P(),
            P("ep", None),
            P("ep", None),
            P("ep", None, "tp"),
            P("ep", None, "tp"),
            P("ep", "tp", None),
            P("ep", "tp"),
            P("ep", "tp"),
            P("tp", "ep"),
            P(),
        ),
        out_specs=(
            P("ep", "tp"),
            P("ep", "tp", None, None),
            P("ep", None, "tp"),
            P("ep", None, "tp"),
            P("ep", None, "tp"),
        ),
        check_vma=False,
    )
```

```python
import functools

import jax
import jax.numpy as jnp
from jax import lax
from jax.experimental import pallas as pl
from jax.experimental.pallas import tpu as pltpu
from jax.sharding import PartitionSpec as P

epsilon = 1e-06


def rms_rows(values, gain):
    return values * lax.rsqrt(jnp.mean(values * values, axis=-1, keepdims=True) + epsilon) * gain


def mixer_kernel(
    tokens_ref,
    gain_ref,
    state_hbm,
    prev_x_ref,
    prev_b_ref,
    prev_c_ref,
    wx_hbm,
    wz_hbm,
    wb_hbm,
    wc_hbm,
    wdt_ref,
    bias_ref,
    a_log_ref,
    skip_ref,
    taps_x_ref,
    taps_b_ref,
    taps_c_ref,
    group_gain_ref,
    mixed_ref,
    state_out,
    next_x_ref,
    next_b_ref,
    next_c_ref,
    wx,
    wz,
    wb,
    wc,
    state,
    w_sem,
    in_sem,
    out_sem,
):
    seqs, heads, head_dim, state_dim = state.shape
    groups = wb.shape[1] // state_dim
    per_group = heads // groups
    inner = heads * head_dim
    fetch = [
        pltpu.make_async_copy(hbm, vmem, w_sem.at[i])
        for i, (hbm, vmem) in enumerate(((wx_hbm, wx), (wb_hbm, wb), (wc_hbm, wc), (wz_hbm, wz)))
    ]
    fetch_state = [
        pltpu.make_async_copy(state_hbm.at[s], state.at[s], in_sem.at[s]) for s in range(seqs)
    ]
    put_state = [
        pltpu.make_async_copy(state.at[s], state_out.at[s], out_sem.at[s]) for s in range(seqs)
    ]
    for copy in fetch[:3] + fetch_state + fetch[3:]:
        copy.start()

    def project(weights):
        out = jnp.dot(normed, weights, preferred_element_type=jnp.float32)
        return out.astype(jnp.bfloat16).astype(jnp.float32)

    def conv(prev_ref, fresh, taps_ref, next_ref):
        prev = prev_ref[...].astype(jnp.float32)
        taps = taps_ref[...].astype(jnp.float32)
        depth = prev.shape[1]
        summed = prev[:, 0, :] * taps[0:1]
        for j in range(1, depth):
            summed = summed + prev[:, j, :] * taps[j : j + 1]
        summed = summed + fresh * taps[depth : depth + 1]
        shifted = jnp.concatenate((prev[:, 1:, :], fresh[:, None, :]), axis=1)
        next_ref[...] = shifted.astype(jnp.bfloat16)
        return jax.nn.silu(summed)

    normed = rms_rows(tokens_ref[...].astype(jnp.float32), gain_ref[...]).astype(jnp.bfloat16)
    all_dt = jnp.dot(normed, wdt_ref[...], preferred_element_type=jnp.float32)
    dt_raw = all_dt[:, :heads]
    for t in range(1, all_dt.shape[1] // heads):
        own = lax.axis_index("tp") == t
        dt_raw = jnp.where(own, all_dt[:, t * heads : (t + 1) * heads], dt_raw)
    step = jax.nn.softplus(dt_raw + bias_ref[...])
    decay = jnp.exp(-step * jnp.exp(a_log_ref[...]))
    spread = lax.broadcasted_iota(jnp.int32, (heads, inner), 1) // head_dim
    spread = spread == lax.broadcasted_iota(jnp.int32, (heads, inner), 0)
    per_head = jnp.concatenate((step, jnp.broadcast_to(skip_ref[...], step.shape)), axis=0)
    wide = jnp.dot(
        per_head,
        spread.astype(jnp.float32),
        precision=lax.Precision.HIGHEST,
        preferred_element_type=jnp.float32,
    )

    fetch[0].wait()
    xs = conv(prev_x_ref, project(wx[...]), taps_x_ref, next_x_ref)
    fetch[1].wait()
    bs = conv(prev_b_ref, project(wb[...]), taps_b_ref, next_b_ref)
    fetch[2].wait()
    cs = conv(prev_c_ref, project(wc[...]), taps_c_ref, next_c_ref)
    stepped = jnp.transpose(wide[:seqs] * xs)
    cs_high = cs.astype(jnp.bfloat16)
    cs_low = (cs - cs_high.astype(jnp.float32)).astype(jnp.bfloat16)
    cs_pair = jnp.concatenate((cs_high, cs_low), axis=0)

    row = lax.broadcasted_iota(jnp.int32, (seqs, per_group * head_dim), 0)
    read = [jnp.zeros(row.shape, jnp.float32) for _ in range(groups)]
    for s in range(seqs):
        fetch_state[s].wait()
        for g in range(groups):
            span = slice(g * state_dim, (g + 1) * state_dim)
            fresh = []
            for h in range(g * per_group, (g + 1) * per_group):
                new = (
                    decay[s : s + 1, h : h + 1] * state[s, h]
                    + stepped[h * head_dim : (h + 1) * head_dim, s : s + 1] * bs[s : s + 1, span]
                )
                state[s, h] = new
                fresh.append(new.astype(jnp.bfloat16))
            both = lax.dot_general(
                cs_pair[:, span],
                jnp.concatenate(fresh, axis=0),
                (((1,), (1,)), ((), ())),
                preferred_element_type=jnp.float32,
            )
            read[g] = jnp.where(row == s, both[:seqs] + both[seqs:], read[g])
        if s > 0:
            put_state[s - 1].start()
    fetch[3].wait()
    gate = jax.nn.silu(project(wz[...]))
    put_state[seqs - 1].start()
    gated = (jnp.concatenate(read, axis=1) + wide[seqs:] * xs) * gate
    block = inner // groups
    for g in range(groups):
        span = slice(g * block, (g + 1) * block)
        part = gated[:, span]
        part = part * lax.rsqrt(jnp.mean(part * part, axis=-1, keepdims=True) + epsilon)
        mixed_ref[:, span] = (part * group_gain_ref[:, span]).astype(jnp.bfloat16)
    for copy in put_state:
        copy.wait()


def mixer(
    tokens,
    norm1_gain,
    ssm_state,
    conv_x,
    conv_b,
    conv_c,
    w_x,
    w_z,
    w_b,
    w_c,
    w_dt,
    dt_bias,
    a_log,
    d_skip,
    taps_x,
    taps_b,
    taps_c,
    group_gain,
):
    seqs = tokens.shape[0]
    vmem = pl.BlockSpec(memory_space=pltpu.VMEM)
    hbm = pl.BlockSpec(memory_space=pl.ANY)
    shape = jax.ShapeDtypeStruct
    return pl.pallas_call(
        mixer_kernel,
        out_shape=(
            shape((seqs, w_x.shape[1]), jnp.bfloat16),
            shape(ssm_state.shape, ssm_state.dtype),
            shape(conv_x.shape, conv_x.dtype),
            shape(conv_b.shape, conv_b.dtype),
            shape(conv_c.shape, conv_c.dtype),
        ),
        in_specs=[vmem, vmem, hbm, vmem, vmem, vmem, hbm, hbm, hbm, hbm] + [vmem] * 8,
        out_specs=(vmem, hbm, vmem, vmem, vmem),
        scratch_shapes=[
            pltpu.VMEM(w_x.shape, jnp.bfloat16),
            pltpu.VMEM(w_z.shape, jnp.bfloat16),
            pltpu.VMEM(w_b.shape, jnp.bfloat16),
            pltpu.VMEM(w_c.shape, jnp.bfloat16),
            pltpu.VMEM(ssm_state.shape, jnp.float32),
            pltpu.SemaphoreType.DMA((4,)),
            pltpu.SemaphoreType.DMA((seqs,)),
            pltpu.SemaphoreType.DMA((seqs,)),
        ],
        compiler_params=pltpu.CompilerParams(vmem_limit_bytes=48 * 1024 * 1024),
        cost_estimate=pl.CostEstimate(flops=10**8, bytes_accessed=14 * 10**6, transcendentals=0),
    )(
        tokens,
        norm1_gain[None],
        ssm_state,
        conv_x,
        conv_b,
        conv_c,
        w_x,
        w_z,
        w_b,
        w_c,
        w_dt,
        dt_bias[None],
        a_log[None],
        d_skip[None],
        taps_x,
        taps_b,
        taps_c,
        group_gain[None],
    )


def tail_kernel(
    peers,
    splits,
    share,
    mixed_ref,
    w_out_hbm,
    tokens_ref,
    gain_ref,
    ids_ref,
    weights_ref,
    gate_hbm,
    up_hbm,
    down_hbm,
    stage_ref,
    branch_ref,
    out_ref,
    w_out,
    gate_up,
    down,
    partials,
    features,
    tables,
    dense,
    packed,
    returned,
    load_sem,
    part_send,
    part_recv,
    feat_send,
    feat_recv,
    table_send,
    table_recv,
    dense_send,
    dense_recv,
    ret_send,
    ret_recv,
):
    ep = lax.axis_index("ep")
    tp = lax.axis_index("tp")
    everyone = peers * splits
    me = ep * splits + tp
    seqs, width = tokens_ref.shape
    hidden = down.shape[0]
    part = width // splits

    loads = [
        pltpu.make_async_copy(w_out_hbm, w_out, load_sem.at[0]),
        pltpu.make_async_copy(gate_hbm.at[0], gate_up.at[:, pl.ds(0, hidden)], load_sem.at[1]),
        pltpu.make_async_copy(up_hbm.at[0], gate_up.at[:, pl.ds(hidden, hidden)], load_sem.at[2]),
        pltpu.make_async_copy(down_hbm.at[0], down, load_sem.at[3]),
    ]
    for load in loads:
        load.start()

    barrier = pltpu.get_barrier_semaphore()

    def greet(i, carry):
        other = lax.rem(me + i, everyone)
        pl.semaphore_signal(
            barrier,
            inc=1,
            device_id={"ep": other // splits, "tp": lax.rem(other, splits)},
            device_id_type=pl.DeviceIdType.MESH,
        )
        return carry

    lax.fori_loop(1, everyone, greet, 0)

    lanes = lax.broadcasted_iota(jnp.int32, tables.shape[1:], 1)
    table = jnp.zeros(tables.shape[1:], jnp.float32)
    for k in range(ids_ref.shape[1]):
        table = table + jnp.where(lanes == ids_ref[:, k : k + 1], weights_ref[:, k : k + 1], 0.0)
    tables[ep] = table
    dense[ep] = stage_ref[ep]

    loads[0].wait()
    partial_out = jnp.dot(mixed_ref[...], w_out[...], preferred_element_type=jnp.float32)
    partials[tp] = partial_out.astype(jnp.bfloat16)

    pl.semaphore_wait(barrier, everyone - 1)

    def part_copy(i, slot):
        return pltpu.make_async_remote_copy(
            src_ref=partials.at[slot],
            dst_ref=partials.at[slot],
            send_sem=part_send.at[i],
            recv_sem=part_recv.at[slot],
            device_id={"ep": ep, "tp": lax.rem(tp + i, splits)},
            device_id_type=pl.DeviceIdType.MESH,
        )

    def table_copy(i, slot):
        return pltpu.make_async_remote_copy(
            src_ref=tables.at[slot],
            dst_ref=tables.at[slot],
            send_sem=table_send.at[i],
            recv_sem=table_recv.at[slot],
            device_id={"ep": lax.rem(ep + i, peers), "tp": tp},
            device_id_type=pl.DeviceIdType.MESH,
        )

    def dense_copy(i, slot):
        return pltpu.make_async_remote_copy(
            src_ref=stage_ref.at[lax.rem(ep + i, peers)],
            dst_ref=dense.at[slot],
            send_sem=dense_send.at[i],
            recv_sem=dense_recv.at[slot],
            device_id={"ep": lax.rem(ep + i, peers), "tp": tp},
            device_id_type=pl.DeviceIdType.MESH,
        )

    def feat_copy(i, slot):
        return pltpu.make_async_remote_copy(
            src_ref=features.at[slot],
            dst_ref=features.at[slot],
            send_sem=feat_send.at[i],
            recv_sem=feat_recv.at[slot],
            device_id={"ep": lax.rem(ep + i, peers), "tp": tp},
            device_id_type=pl.DeviceIdType.MESH,
        )

    def ret_copy(i, slot):
        other = lax.rem(me + i, everyone)
        return pltpu.make_async_remote_copy(
            src_ref=packed.at[lax.rem(other, splits), other // splits],
            dst_ref=returned.at[slot],
            send_sem=ret_send.at[i],
            recv_sem=ret_recv.at[slot],
            device_id={"ep": other // splits, "tp": lax.rem(other, splits)},
            device_id_type=pl.DeviceIdType.MESH,
        )

    def start_all(copy, slot, count):
        def step(i, carry):
            copy(i, slot).start()
            return carry

        lax.fori_loop(1, count, step, 0)

    def take_all(copy, own, count):
        def step(i, carry):
            copy(i, lax.rem(own + count - i, count)).wait_recv()
            return carry

        lax.fori_loop(1, count, step, 0)

    def sent_all(copy, slot, count):
        def step(i, carry):
            copy(i, slot).wait_send()
            return carry

        lax.fori_loop(1, count, step, 0)

    start_all(part_copy, tp, splits)
    start_all(table_copy, ep, peers)
    start_all(dense_copy, ep, peers)

    take_all(part_copy, tp, splits)
    summed = partials[0].astype(jnp.float32)
    for t in range(1, splits):
        summed = summed + partials[t].astype(jnp.float32)
    residual = (tokens_ref[...].astype(jnp.float32) + summed).astype(jnp.bfloat16)
    residual = residual.astype(jnp.float32)
    normed2 = rms_rows(residual, gain_ref[...]).astype(jnp.bfloat16)
    features[ep] = normed2
    start_all(feat_copy, ep, peers)

    take_all(table_copy, ep, peers)
    take_all(dense_copy, ep, peers)
    every_table = tables[...].reshape(peers * seqs, tables.shape[2])
    columns = lax.broadcasted_iota(jnp.int32, every_table.shape, 1)
    own_weight = jnp.sum(jnp.where(columns == ep, every_table, 0.0), axis=1, keepdims=True)
    dense_weights = dense[...].reshape(width, dense.shape[2])
    for load in loads[1:]:
        load.wait()

    take_all(feat_copy, ep, peers)
    rows = features[...].astype(jnp.float32).reshape(peers * seqs, width)
    rows16 = rows.astype(jnp.bfloat16)
    pre = jnp.dot(rows16, gate_up[...], preferred_element_type=jnp.float32)
    active = own_weight * (jax.nn.silu(pre[:, :hidden]) * pre[:, hidden:])
    dense_pre = jnp.dot(rows16, dense_weights, preferred_element_type=jnp.float32)
    branch = jax.nn.sigmoid(
        jnp.sum(rows * branch_ref[...].astype(jnp.float32), axis=1, keepdims=True)
    )
    lane = lax.broadcasted_iota(jnp.int32, dense_pre.shape, 1)
    dense_act = jax.nn.silu(pltpu.roll(dense_pre, 2 * share, 1)) * pltpu.roll(dense_pre, share, 1)
    dense_act = jnp.where((lane >= 2 * share) & (lane < 3 * share), branch * dense_act, 0.0)
    total = jnp.dot(active.astype(jnp.bfloat16), down[...], preferred_element_type=jnp.float32)
    total = total + lax.dot_general(
        dense_act.astype(jnp.bfloat16),
        dense_weights,
        (((1,), (1,)), ((), ())),
        preferred_element_type=jnp.float32,
    )
    for t in range(splits):
        packed[t] = (
            total[:, t * part : (t + 1) * part].reshape(peers, seqs, part).astype(jnp.bfloat16)
        )
    returned[me] = packed[tp, ep]
    start_all(ret_copy, me, everyone)

    sent_all(part_copy, tp, splits)
    sent_all(table_copy, ep, peers)
    sent_all(dense_copy, ep, peers)
    sent_all(feat_copy, ep, peers)
    own_rows = residual[:, :part]
    for t in range(1, splits):
        own_rows = jnp.where(tp == t, residual[:, t * part : (t + 1) * part], own_rows)

    take_all(ret_copy, me, everyone)
    mixed = own_rows + jnp.sum(returned[...].astype(jnp.float32), axis=0)
    out_ref[...] = mixed.astype(jnp.bfloat16)
    sent_all(ret_copy, me, everyone)


def after_mixer(
    mixed_heads,
    w_out,
    tokens,
    norm2_gain,
    route_ids,
    route_weights,
    exp_gate,
    exp_up,
    exp_down,
    dense_gate,
    dense_up,
    dense_down,
    branch_gate,
):
    peers = lax.axis_size("ep")
    splits = lax.axis_size("tp")
    seqs, width = tokens.shape
    depth, local_hidden = dense_gate.shape
    share = local_hidden // peers
    hidden = exp_gate.shape[2]
    part = width // splits
    lanes = -(-3 * share // 128) * 128
    by_owner = lambda w: w.reshape(depth, peers, share).transpose(1, 0, 2)
    stage = jnp.concatenate(
        (
            by_owner(dense_gate),
            by_owner(dense_up),
            dense_down.reshape(peers, share, depth).transpose(0, 2, 1),
            jnp.zeros((peers, depth, lanes - 3 * share), jnp.bfloat16),
        ),
        axis=2,
    )
    vmem = pl.BlockSpec(memory_space=pltpu.VMEM)
    hbm = pl.BlockSpec(memory_space=pl.ANY)
    dma = lambda count: pltpu.SemaphoreType.DMA((count,))
    return pl.pallas_call(
        functools.partial(tail_kernel, peers, splits, share),
        out_shape=jax.ShapeDtypeStruct((seqs, part), jnp.bfloat16),
        in_specs=[vmem, hbm, vmem, vmem, vmem, vmem, hbm, hbm, hbm, vmem, vmem],
        out_specs=vmem,
        scratch_shapes=[
            pltpu.VMEM(w_out.shape, jnp.bfloat16),
            pltpu.VMEM((width, 2 * hidden), jnp.bfloat16),
            pltpu.VMEM((hidden, width), jnp.bfloat16),
            pltpu.VMEM((splits, seqs, width), jnp.bfloat16),
            pltpu.VMEM((peers, seqs, width), jnp.bfloat16),
            pltpu.VMEM((peers, seqs, 128), jnp.float32),
            pltpu.VMEM((peers, depth, lanes), jnp.bfloat16),
            pltpu.VMEM((splits, peers, seqs, part), jnp.bfloat16),
            pltpu.VMEM((peers * splits, seqs, part), jnp.bfloat16),
            dma(4),
            dma(splits),
            dma(splits),
            dma(peers),
            dma(peers),
            dma(peers),
            dma(peers),
            dma(peers),
            dma(peers),
            dma(peers * splits),
            dma(peers * splits),
        ],
        compiler_params=pltpu.CompilerParams(
            collective_id=0, has_side_effects=True, vmem_limit_bytes=32 * 1024 * 1024
        ),
        cost_estimate=pl.CostEstimate(flops=10**9, bytes_accessed=10**7, transcendentals=0),
    )(
        mixed_heads,
        w_out,
        tokens,
        norm2_gain[None],
        route_ids,
        route_weights,
        exp_gate,
        exp_up,
        exp_down,
        stage,
        branch_gate[None],
    )


def body(
    tokens,
    ssm_state,
    conv_x,
    conv_b,
    conv_c,
    w_x,
    w_z,
    w_b,
    w_c,
    w_dt,
    dt_bias,
    a_log,
    d_skip,
    taps_x,
    taps_b,
    taps_c,
    norm1_gain,
    group_gain,
    w_out,
    norm2_gain,
    route_ids,
    route_weights,
    exp_gate,
    exp_up,
    exp_down,
    dense_gate,
    dense_up,
    dense_down,
    branch_gate,
):
    mixed_heads, state_next, conv_x_next, conv_b_next, conv_c_next = mixer(
        tokens,
        norm1_gain,
        ssm_state,
        conv_x,
        conv_b,
        conv_c,
        w_x,
        w_z,
        w_b,
        w_c,
        w_dt,
        dt_bias,
        a_log,
        d_skip,
        taps_x,
        taps_b,
        taps_c,
        group_gain,
    )
    mixed = after_mixer(
        mixed_heads,
        w_out,
        tokens,
        norm2_gain,
        route_ids,
        route_weights,
        exp_gate,
        exp_up,
        exp_down,
        dense_gate,
        dense_up,
        dense_down,
        branch_gate,
    )
    return (mixed, state_next, conv_x_next, conv_b_next, conv_c_next)


def solution(mesh):
    return jax.shard_map(
        body,
        mesh=mesh,
        in_specs=(
            P("ep", None),
            P("ep", "tp", None, None),
            P("ep", None, "tp"),
            P("ep", None, "tp"),
            P("ep", None, "tp"),
            P(None, "tp"),
            P(None, "tp"),
            P(None, "tp"),
            P(None, "tp"),
            P(),
            P("tp"),
            P("tp"),
            P("tp"),
            P(None, "tp"),
            P(None, "tp"),
            P(None, "tp"),
            P(),
            P("tp"),
            P("tp", None),
            P(),
            P("ep", None),
            P("ep", None),
            P("ep", None, "tp"),
            P("ep", None, "tp"),
            P("ep", "tp", None),
            P("ep", "tp"),
            P("ep", "tp"),
            P("tp", "ep"),
            P(),
        ),
        out_specs=(
            P("ep", "tp"),
            P("ep", "tp", None, None),
            P("ep", None, "tp"),
            P("ep", None, "tp"),
            P("ep", None, "tp"),
        ),
        check_vma=False,
    )
```

```python
import functools

import jax
import jax.numpy as jnp
from jax import lax
from jax.experimental import pallas as pl
from jax.experimental.pallas import tpu as pltpu
from jax.sharding import PartitionSpec as P

epsilon = 1e-06


def rms_rows(values, gain):
    return values * lax.rsqrt(jnp.mean(values * values, axis=-1, keepdims=True) + epsilon) * gain


def mixer_kernel(
    tokens_ref,
    gain_ref,
    state_hbm,
    prev_x_ref,
    prev_b_ref,
    prev_c_ref,
    wx_hbm,
    wz_hbm,
    wb_hbm,
    wc_hbm,
    wdt_ref,
    bias_ref,
    a_log_ref,
    skip_ref,
    taps_x_ref,
    taps_b_ref,
    taps_c_ref,
    group_gain_ref,
    mixed_ref,
    state_out,
    next_x_ref,
    next_b_ref,
    next_c_ref,
    wx,
    wz,
    wb,
    wc,
    state,
    w_sem,
    in_sem,
    out_sem,
):
    seqs, heads, head_dim, state_dim = state.shape
    groups = wb.shape[1] // state_dim
    per_group = heads // groups
    inner = heads * head_dim
    fetch = [
        pltpu.make_async_copy(hbm, vmem, w_sem.at[i])
        for i, (hbm, vmem) in enumerate(((wx_hbm, wx), (wb_hbm, wb), (wc_hbm, wc), (wz_hbm, wz)))
    ]
    fetch_state = [
        pltpu.make_async_copy(state_hbm.at[s], state.at[s], in_sem.at[s]) for s in range(seqs)
    ]
    put_state = [
        pltpu.make_async_copy(state.at[s], state_out.at[s], out_sem.at[s]) for s in range(seqs)
    ]
    for copy in fetch[:3] + fetch_state + fetch[3:]:
        copy.start()

    def project(weights):
        out = jnp.dot(normed, weights, preferred_element_type=jnp.float32)
        return out.astype(jnp.bfloat16).astype(jnp.float32)

    def conv(prev_ref, fresh, taps_ref, next_ref):
        prev = prev_ref[...].astype(jnp.float32)
        taps = taps_ref[...].astype(jnp.float32)
        depth = prev.shape[0]
        summed = prev[0] * taps[0:1]
        for j in range(1, depth):
            summed = summed + prev[j] * taps[j : j + 1]
            next_ref[j - 1] = prev[j].astype(jnp.bfloat16)
        summed = summed + fresh * taps[depth : depth + 1]
        next_ref[depth - 1] = fresh.astype(jnp.bfloat16)
        return jax.nn.silu(summed)

    normed = rms_rows(tokens_ref[...].astype(jnp.float32), gain_ref[...]).astype(jnp.bfloat16)
    all_dt = lax.dot_general(
        normed, wdt_ref[...], (((1,), (1,)), ((), ())), preferred_element_type=jnp.float32
    )
    dt_raw = all_dt[:, :heads]
    for t in range(1, all_dt.shape[1] // heads):
        own = lax.axis_index("tp") == t
        dt_raw = jnp.where(own, all_dt[:, t * heads : (t + 1) * heads], dt_raw)
    step = jax.nn.softplus(dt_raw + bias_ref[...])
    decay = jnp.exp(-step * jnp.exp(a_log_ref[...]))
    spread = lax.broadcasted_iota(jnp.int32, (heads, inner), 1) // head_dim
    spread = spread == lax.broadcasted_iota(jnp.int32, (heads, inner), 0)
    per_head = jnp.concatenate((step, jnp.broadcast_to(skip_ref[...], step.shape)), axis=0)
    wide = jnp.dot(
        per_head,
        spread.astype(jnp.float32),
        precision=lax.Precision.HIGHEST,
        preferred_element_type=jnp.float32,
    )

    fetch[0].wait()
    xs = conv(prev_x_ref, project(wx[...]), taps_x_ref, next_x_ref)
    fetch[1].wait()
    bs = conv(prev_b_ref, project(wb[...]), taps_b_ref, next_b_ref)
    fetch[2].wait()
    cs = conv(prev_c_ref, project(wc[...]), taps_c_ref, next_c_ref)
    stepped = jnp.transpose(wide[:seqs] * xs)
    cs_high = cs.astype(jnp.bfloat16)
    cs_low = (cs - cs_high.astype(jnp.float32)).astype(jnp.bfloat16)
    cs_pair = jnp.concatenate((cs_high, cs_low), axis=0)

    row = lax.broadcasted_iota(jnp.int32, (seqs, per_group * head_dim), 0)
    read = [jnp.zeros(row.shape, jnp.float32) for _ in range(groups)]
    for s in range(seqs):
        fetch_state[s].wait()
        for g in range(groups):
            span = slice(g * state_dim, (g + 1) * state_dim)
            fresh = []
            for h in range(g * per_group, (g + 1) * per_group):
                new = (
                    decay[s : s + 1, h : h + 1] * state[s, h]
                    + stepped[h * head_dim : (h + 1) * head_dim, s : s + 1] * bs[s : s + 1, span]
                )
                state[s, h] = new
                fresh.append(new.astype(jnp.bfloat16))
            both = lax.dot_general(
                cs_pair[:, span],
                jnp.concatenate(fresh, axis=0),
                (((1,), (1,)), ((), ())),
                preferred_element_type=jnp.float32,
            )
            read[g] = jnp.where(row == s, both[:seqs] + both[seqs:], read[g])
        if s > 0:
            put_state[s - 1].start()
    fetch[3].wait()
    gate = jax.nn.silu(project(wz[...]))
    put_state[seqs - 1].start()
    gated = (jnp.concatenate(read, axis=1) + wide[seqs:] * xs) * gate
    block = inner // groups
    for g in range(groups):
        span = slice(g * block, (g + 1) * block)
        part = gated[:, span]
        part = part * lax.rsqrt(jnp.mean(part * part, axis=-1, keepdims=True) + epsilon)
        mixed_ref[:, span] = (part * group_gain_ref[:, span]).astype(jnp.bfloat16)
    for copy in put_state:
        copy.wait()


def mixer(
    tokens,
    norm1_gain,
    ssm_state,
    conv_x,
    conv_b,
    conv_c,
    w_x,
    w_z,
    w_b,
    w_c,
    w_dt,
    dt_bias,
    a_log,
    d_skip,
    taps_x,
    taps_b,
    taps_c,
    group_gain,
):
    seqs = tokens.shape[0]
    vmem = pl.BlockSpec(memory_space=pltpu.VMEM)
    hbm = pl.BlockSpec(memory_space=pl.ANY)
    shape = jax.ShapeDtypeStruct
    taps_first = lambda a: a.transpose(1, 0, 2)
    conv_x, conv_b, conv_c = taps_first(conv_x), taps_first(conv_b), taps_first(conv_c)
    mixed, state, next_x, next_b, next_c = pl.pallas_call(
        mixer_kernel,
        out_shape=(
            shape((seqs, w_x.shape[1]), jnp.bfloat16),
            shape(ssm_state.shape, ssm_state.dtype),
            shape(conv_x.shape, conv_x.dtype),
            shape(conv_b.shape, conv_b.dtype),
            shape(conv_c.shape, conv_c.dtype),
        ),
        in_specs=[vmem, vmem, hbm, vmem, vmem, vmem, hbm, hbm, hbm, hbm] + [vmem] * 8,
        out_specs=(vmem, hbm, vmem, vmem, vmem),
        scratch_shapes=[
            pltpu.VMEM(w_x.shape, jnp.bfloat16),
            pltpu.VMEM(w_z.shape, jnp.bfloat16),
            pltpu.VMEM(w_b.shape, jnp.bfloat16),
            pltpu.VMEM(w_c.shape, jnp.bfloat16),
            pltpu.VMEM(ssm_state.shape, jnp.float32),
            pltpu.SemaphoreType.DMA((4,)),
            pltpu.SemaphoreType.DMA((seqs,)),
            pltpu.SemaphoreType.DMA((seqs,)),
        ],
        cost_estimate=pl.CostEstimate(flops=10**8, bytes_accessed=14 * 10**6, transcendentals=0),
    )(
        tokens,
        norm1_gain[None],
        ssm_state,
        conv_x,
        conv_b,
        conv_c,
        w_x,
        w_z,
        w_b,
        w_c,
        w_dt.T,
        dt_bias[None],
        a_log[None],
        d_skip[None],
        taps_x,
        taps_b,
        taps_c,
        group_gain[None],
    )
    return mixed, state, taps_first(next_x), taps_first(next_b), taps_first(next_c)


def tail_kernel(
    peers,
    splits,
    share,
    mixed_ref,
    w_out_hbm,
    tokens_ref,
    gain_ref,
    ids_ref,
    weights_ref,
    gate_hbm,
    up_hbm,
    down_hbm,
    dense_gate_ref,
    dense_up_ref,
    dense_down_ref,
    branch_ref,
    out_ref,
    w_out,
    gate_up,
    down,
    partials,
    features,
    tables,
    stage_ref,
    dense,
    packed,
    returned,
    load_sem,
    part_send,
    part_recv,
    feat_send,
    feat_recv,
    table_send,
    table_recv,
    dense_send,
    dense_recv,
    ret_send,
    ret_recv,
):
    ep = lax.axis_index("ep")
    tp = lax.axis_index("tp")
    everyone = peers * splits
    me = ep * splits + tp
    seqs, width = tokens_ref.shape
    hidden = down.shape[0]
    part = width // splits

    loads = [
        pltpu.make_async_copy(w_out_hbm, w_out, load_sem.at[0]),
        pltpu.make_async_copy(gate_hbm.at[0], gate_up.at[:, pl.ds(0, hidden)], load_sem.at[1]),
        pltpu.make_async_copy(up_hbm.at[0], gate_up.at[:, pl.ds(hidden, hidden)], load_sem.at[2]),
        pltpu.make_async_copy(down_hbm.at[0], down, load_sem.at[3]),
    ]
    for load in loads:
        load.start()

    barrier = pltpu.get_barrier_semaphore()

    def greet(i, carry):
        other = lax.rem(me + i, everyone)
        pl.semaphore_signal(
            barrier,
            inc=1,
            device_id={"ep": other // splits, "tp": lax.rem(other, splits)},
            device_id_type=pl.DeviceIdType.MESH,
        )
        return carry

    lax.fori_loop(1, everyone, greet, 0)

    lanes = lax.broadcasted_iota(jnp.int32, tables.shape[1:], 1)
    table = jnp.zeros(tables.shape[1:], jnp.float32)
    for k in range(ids_ref.shape[1]):
        table = table + jnp.where(lanes == ids_ref[:, k : k + 1], weights_ref[:, k : k + 1], 0.0)
    tables[ep] = table
    lane = lax.broadcasted_iota(jnp.int32, stage_ref.shape[1:], 1)
    for owner in range(peers):
        start = owner * share
        base = start // 128 * 128
        block = jnp.zeros(stage_ref.shape[1:], jnp.float32)
        for i, ref in enumerate((dense_gate_ref, dense_up_ref, dense_down_ref)):
            source = ref[:, base : base + 128].astype(jnp.float32)
            shift = (i * share - (start - base)) % 128
            if shift:
                source = pltpu.roll(source, shift, 1)
            block = jnp.where((lane >= i * share) & (lane < (i + 1) * share), source, block)
        stage_ref[owner] = block.astype(jnp.bfloat16)
    dense[ep] = stage_ref[ep]

    loads[0].wait()
    partial_out = jnp.dot(mixed_ref[...], w_out[...], preferred_element_type=jnp.float32)
    partials[tp] = partial_out.astype(jnp.bfloat16)

    pl.semaphore_wait(barrier, everyone - 1)

    def part_copy(i, slot):
        return pltpu.make_async_remote_copy(
            src_ref=partials.at[slot],
            dst_ref=partials.at[slot],
            send_sem=part_send.at[i],
            recv_sem=part_recv.at[slot],
            device_id={"ep": ep, "tp": lax.rem(tp + i, splits)},
            device_id_type=pl.DeviceIdType.MESH,
        )

    def table_copy(i, slot):
        return pltpu.make_async_remote_copy(
            src_ref=tables.at[slot],
            dst_ref=tables.at[slot],
            send_sem=table_send.at[i],
            recv_sem=table_recv.at[slot],
            device_id={"ep": lax.rem(ep + i, peers), "tp": tp},
            device_id_type=pl.DeviceIdType.MESH,
        )

    def dense_copy(i, slot):
        return pltpu.make_async_remote_copy(
            src_ref=stage_ref.at[lax.rem(ep + i, peers)],
            dst_ref=dense.at[slot],
            send_sem=dense_send.at[i],
            recv_sem=dense_recv.at[slot],
            device_id={"ep": lax.rem(ep + i, peers), "tp": tp},
            device_id_type=pl.DeviceIdType.MESH,
        )

    def feat_copy(i, slot):
        return pltpu.make_async_remote_copy(
            src_ref=features.at[slot],
            dst_ref=features.at[slot],
            send_sem=feat_send.at[i],
            recv_sem=feat_recv.at[slot],
            device_id={"ep": lax.rem(ep + i, peers), "tp": tp},
            device_id_type=pl.DeviceIdType.MESH,
        )

    def ret_copy(i, slot):
        other = lax.rem(me + i, everyone)
        return pltpu.make_async_remote_copy(
            src_ref=packed.at[lax.rem(other, splits), other // splits],
            dst_ref=returned.at[slot],
            send_sem=ret_send.at[i],
            recv_sem=ret_recv.at[slot],
            device_id={"ep": other // splits, "tp": lax.rem(other, splits)},
            device_id_type=pl.DeviceIdType.MESH,
        )

    def start_all(copy, slot, count):
        def step(i, carry):
            copy(i, slot).start()
            return carry

        lax.fori_loop(1, count, step, 0)

    def take_all(copy, own, count):
        def step(i, carry):
            copy(i, lax.rem(own + count - i, count)).wait_recv()
            return carry

        lax.fori_loop(1, count, step, 0)

    def sent_all(copy, slot, count):
        def step(i, carry):
            copy(i, slot).wait_send()
            return carry

        lax.fori_loop(1, count, step, 0)

    start_all(part_copy, tp, splits)
    start_all(table_copy, ep, peers)
    start_all(dense_copy, ep, peers)

    take_all(part_copy, tp, splits)
    summed = partials[0].astype(jnp.float32)
    for t in range(1, splits):
        summed = summed + partials[t].astype(jnp.float32)
    residual = (tokens_ref[...].astype(jnp.float32) + summed).astype(jnp.bfloat16)
    residual = residual.astype(jnp.float32)
    normed2 = rms_rows(residual, gain_ref[...]).astype(jnp.bfloat16)
    features[ep] = normed2
    start_all(feat_copy, ep, peers)

    take_all(table_copy, ep, peers)
    take_all(dense_copy, ep, peers)
    every_table = tables[...].reshape(peers * seqs, tables.shape[2])
    columns = lax.broadcasted_iota(jnp.int32, every_table.shape, 1)
    own_weight = jnp.sum(jnp.where(columns == ep, every_table, 0.0), axis=1, keepdims=True)
    dense_weights = dense[...].reshape(width, dense.shape[2])
    for load in loads[1:]:
        load.wait()

    take_all(feat_copy, ep, peers)
    rows = features[...].astype(jnp.float32).reshape(peers * seqs, width)
    rows16 = rows.astype(jnp.bfloat16)
    pre = jnp.dot(rows16, gate_up[...], preferred_element_type=jnp.float32)
    active = own_weight * (jax.nn.silu(pre[:, :hidden]) * pre[:, hidden:])
    dense_pre = jnp.dot(rows16, dense_weights, preferred_element_type=jnp.float32)
    branch = jax.nn.sigmoid(
        jnp.sum(rows * branch_ref[...].astype(jnp.float32), axis=1, keepdims=True)
    )
    lane = lax.broadcasted_iota(jnp.int32, dense_pre.shape, 1)
    dense_act = jax.nn.silu(pltpu.roll(dense_pre, 2 * share, 1)) * pltpu.roll(dense_pre, share, 1)
    dense_act = jnp.where((lane >= 2 * share) & (lane < 3 * share), branch * dense_act, 0.0)
    total = jnp.dot(active.astype(jnp.bfloat16), down[...], preferred_element_type=jnp.float32)
    total = total + lax.dot_general(
        dense_act.astype(jnp.bfloat16),
        dense_weights,
        (((1,), (1,)), ((), ())),
        preferred_element_type=jnp.float32,
    )
    for t in range(splits):
        packed[t] = (
            total[:, t * part : (t + 1) * part].reshape(peers, seqs, part).astype(jnp.bfloat16)
        )
    returned[me] = packed[tp, ep]
    start_all(ret_copy, me, everyone)

    sent_all(part_copy, tp, splits)
    sent_all(table_copy, ep, peers)
    sent_all(dense_copy, ep, peers)
    sent_all(feat_copy, ep, peers)
    own_rows = residual[:, :part]
    for t in range(1, splits):
        own_rows = jnp.where(tp == t, residual[:, t * part : (t + 1) * part], own_rows)

    take_all(ret_copy, me, everyone)
    mixed = own_rows + jnp.sum(returned[...].astype(jnp.float32), axis=0)
    out_ref[...] = mixed.astype(jnp.bfloat16)
    sent_all(ret_copy, me, everyone)


def after_mixer(
    mixed_heads,
    w_out,
    tokens,
    norm2_gain,
    route_ids,
    route_weights,
    exp_gate,
    exp_up,
    exp_down,
    dense_gate,
    dense_up,
    dense_down,
    branch_gate,
):
    peers = lax.axis_size("ep")
    splits = lax.axis_size("tp")
    seqs, width = tokens.shape
    depth, local_hidden = dense_gate.shape
    share = local_hidden // peers
    hidden = exp_gate.shape[2]
    part = width // splits
    lanes = -(-3 * share // 128) * 128
    vmem = pl.BlockSpec(memory_space=pltpu.VMEM)
    hbm = pl.BlockSpec(memory_space=pl.ANY)
    dma = lambda count: pltpu.SemaphoreType.DMA((count,))
    return pl.pallas_call(
        functools.partial(tail_kernel, peers, splits, share),
        out_shape=jax.ShapeDtypeStruct((seqs, part), jnp.bfloat16),
        in_specs=[vmem, hbm, vmem, vmem, vmem, vmem, hbm, hbm, hbm, vmem, vmem, vmem, vmem],
        out_specs=vmem,
        scratch_shapes=[
            pltpu.VMEM(w_out.shape, jnp.bfloat16),
            pltpu.VMEM((width, 2 * hidden), jnp.bfloat16),
            pltpu.VMEM((hidden, width), jnp.bfloat16),
            pltpu.VMEM((splits, seqs, width), jnp.bfloat16),
            pltpu.VMEM((peers, seqs, width), jnp.bfloat16),
            pltpu.VMEM((peers, seqs, 128), jnp.float32),
            pltpu.VMEM((peers, depth, lanes), jnp.bfloat16),
            pltpu.VMEM((peers, depth, lanes), jnp.bfloat16),
            pltpu.VMEM((splits, peers, seqs, part), jnp.bfloat16),
            pltpu.VMEM((peers * splits, seqs, part), jnp.bfloat16),
            dma(4),
            dma(splits),
            dma(splits),
            dma(peers),
            dma(peers),
            dma(peers),
            dma(peers),
            dma(peers),
            dma(peers),
            dma(peers * splits),
            dma(peers * splits),
        ],
        compiler_params=pltpu.CompilerParams(
            collective_id=0, has_side_effects=True
        ),
        cost_estimate=pl.CostEstimate(flops=10**9, bytes_accessed=10**7, transcendentals=0),
    )(
        mixed_heads,
        w_out,
        tokens,
        norm2_gain[None],
        route_ids,
        route_weights,
        exp_gate,
        exp_up,
        exp_down,
        dense_gate,
        dense_up,
        dense_down.T,
        branch_gate.astype(jnp.float32)[None],
    )


def body(
    tokens,
    ssm_state,
    conv_x,
    conv_b,
    conv_c,
    w_x,
    w_z,
    w_b,
    w_c,
    w_dt,
    dt_bias,
    a_log,
    d_skip,
    taps_x,
    taps_b,
    taps_c,
    norm1_gain,
    group_gain,
    w_out,
    norm2_gain,
    route_ids,
    route_weights,
    exp_gate,
    exp_up,
    exp_down,
    dense_gate,
    dense_up,
    dense_down,
    branch_gate,
):
    mixed_heads, state_next, conv_x_next, conv_b_next, conv_c_next = mixer(
        tokens,
        norm1_gain,
        ssm_state,
        conv_x,
        conv_b,
        conv_c,
        w_x,
        w_z,
        w_b,
        w_c,
        w_dt,
        dt_bias,
        a_log,
        d_skip,
        taps_x,
        taps_b,
        taps_c,
        group_gain,
    )
    mixed = after_mixer(
        mixed_heads,
        w_out,
        tokens,
        norm2_gain,
        route_ids,
        route_weights,
        exp_gate,
        exp_up,
        exp_down,
        dense_gate,
        dense_up,
        dense_down,
        branch_gate,
    )
    return (mixed, state_next, conv_x_next, conv_b_next, conv_c_next)


def solution(mesh):
    return jax.shard_map(
        body,
        mesh=mesh,
        in_specs=(
            P("ep", None),
            P("ep", "tp", None, None),
            P("ep", None, "tp"),
            P("ep", None, "tp"),
            P("ep", None, "tp"),
            P(None, "tp"),
            P(None, "tp"),
            P(None, "tp"),
            P(None, "tp"),
            P(),
            P("tp"),
            P("tp"),
            P("tp"),
            P(None, "tp"),
            P(None, "tp"),
            P(None, "tp"),
            P(),
            P("tp"),
            P("tp", None),
            P(),
            P("ep", None),
            P("ep", None),
            P("ep", None, "tp"),
            P("ep", None, "tp"),
            P("ep", "tp", None),
            P("ep", "tp"),
            P("ep", "tp"),
            P("tp", "ep"),
            P(),
        ),
        out_specs=(
            P("ep", "tp"),
            P("ep", "tp", None, None),
            P("ep", None, "tp"),
            P("ep", None, "tp"),
            P("ep", None, "tp"),
        ),
        check_vma=False,
    )
```
